32 devices in a mesh: ep: 8 (over z, y), tp: 4 (over x, core).
Axes of the slice: x: 2, y: 2, z: 4, core: 2. Of those that a mesh axis runs over, the one named last changes fastest.
Arguments:
- pool_input: bfloat16 [12288, 2048], P('ep', 'tp'), may hold values from -6 to 6
- group_mix: bfloat16 [4, 512, 512], P('tp'), may hold values from -0.25 to 0.25
- group_scale: float32 [2048], P('tp'), may hold values from 0.1 to 1.9
- out_proj: bfloat16 [2048, 2048], replicated, may hold values from -0.125 to 0.125
- moe_input: bfloat16 [4096, 2048], P(('ep', 'tp')), may hold values from -6 to 6
- norm_gain: float32 [2048], replicated, may hold values from 0.1 to 1.9
- expert_ids: int32 [4096, 2], P(('ep', 'tp')), may hold values from 0 to 31, all different within a row; in each aligned block of 128 rows (0 to 127, 128 to 255, ...) at most 16 rows name the same one
- expert_scores: float32 [4096, 2], P(('ep', 'tp')), may hold values from 0.1 to 1
- gate_proj: bfloat16 [32, 2048, 1024], P(('ep', 'tp')), may hold values from -0.125 to 0.125
- up_proj: bfloat16 [32, 2048, 1024], P(('ep', 'tp')), may hold values from -0.125 to 0.125
- down_proj: bfloat16 [32, 1024, 2048], P(('ep', 'tp')), may hold values from -0.1875 to 0.1875
Outputs:
- mixed_tokens: bfloat16 [12288, 2048], P(('ep', 'tp'))
- mixed_experts: bfloat16 [4096, 2048], P(('ep', 'tp'))
The draws below stay inside these ranges and needn't reach their ends.
Inputs may be any that keep to these rules, and one draw needn't show every extreme that they name: `expert_ids`: each row names 2 different experts. Within the 128 rows of one device (aligned blocks) no expert is named by more than 16 rows, a bound that some block reaches of some device.
All inputs are finite; a program needn't handle non-finite values.
Results may differ from the reference program's by a relative error of at most 0.012.
Values may be sent and summed in bfloat16 or wider, within the bound.
A program may use at most 128 MiB of HBM per device.

```python
import math
import jax
import jax.numpy as jnp
import numpy as np
from jax import lax

D = 2048
GROUPS = 4
FF = 1024
TOPK = 2
TOK_B_DEV = 128
GW = 512
TOKENS_A = 12288
TOKENS_B = 4096
EXPERTS = 32
CAP = 16
N_EP = 8
N_TP = 4


def block_levels(own_key, shape, cuts, smallest, largest):
    factor_of = 1.0
    for axis_at, blocks in cuts:
        draws = jax.random.uniform(jax.random.fold_in(jax.random.fold_in(own_key, 6), axis_at), (blocks,), jnp.float32, smallest / len(cuts), largest / len(cuts))
        factor_of = factor_of * jnp.repeat(jnp.exp(draws), shape[axis_at] // blocks).reshape((-1,) + (1,) * (len(shape) - 1 - axis_at))
    return factor_of


def shared_out(stream_key, own, number, rows, number_of, top, bound, skew):
    order = jax.random.permutation(stream_key, number_of)
    crowded, common = load_shares(number_of, rows * top, bound, skew, True), load_shares(number_of, rows * top, bound, skew, False)
    places = jnp.arange(number_of)

    def named(lengths, offset_by):
        used = int((lengths > 0).sum())
        fixed = max(1, used // 4)
        passed = fixed + (places - fixed + offset_by * (used - fixed)) % max(1, number_of - fixed)
        return jnp.zeros((number_of,), jnp.int32).at[order[jnp.where(places < fixed, places, passed)]].set(jnp.asarray(lengths, jnp.int32))

    lengths = jnp.where(number % 4 == 0, named(crowded, number // 4), named(common, number - number // 4 - 1))
    mixed = jax.random.permutation(jax.random.fold_in(own, 3), number_of)
    giver, receiver = mixed[0:number_of // 2 * 2:2], mixed[1:number_of // 2 * 2:2]
    margin = jnp.minimum(lengths[giver] - 1, bound - lengths[receiver]) // 2
    margin = jnp.where((giver == order[0]) | (receiver == order[0]) | (lengths[receiver] == 0), 0, jnp.maximum(margin, 0))
    passed = jax.random.randint(jax.random.fold_in(own, 4), (number_of // 2,), 0, 1 << 20) % (margin + 1)
    lengths = lengths.at[giver].add(-passed).at[receiver].add(passed)
    labels = jnp.searchsorted(jnp.cumsum(lengths), jnp.arange(rows * top), side="right").astype(jnp.int32)
    listing = labels.reshape(top, rows).T
    listing = listing[jax.random.permutation(jax.random.fold_in(own, 1), rows)]
    offset_by = jax.random.randint(jax.random.fold_in(own, 2), (rows, 1), 0, top)
    return jnp.take_along_axis(listing, (jnp.arange(top)[None, :] + offset_by) % top, axis=1)


def load_shares(count, total, limit, skew, full):
    loads = [(1 << 20) // math.isqrt(rank ** skew) + 1 for rank in range(1, count + 1)]
    largest = limit if full else min(limit, max(-(-total // count), total * loads[0] // sum(loads)))
    least = 1 if total - largest >= count - 1 else 0
    given, spare = [largest] + [least] * (count - 1), total - largest - least * (count - 1)
    while spare > 0:
        candidates = [i for i in range(1, count) if given[i] < largest] or [i for i in range(1, count) if given[i] < limit]
        whole, remaining = sum([loads[i] for i in candidates]), spare
        for i in candidates:
            extra = min(limit - given[i], max(1, remaining * loads[i] // whole), spare)
            given[i] = given[i] + extra
            spare = spare - extra
    return np.array(given)


def normal_values(stream_key, extent, deviation, limit, cuts=(), kind=jnp.bfloat16):
    values = deviation * jax.random.normal(stream_key, extent, jnp.float32)
    if cuts:
        values = values * block_levels(stream_key, extent, cuts, -0.22, 0.18)
    return jnp.clip(values, -limit, limit).astype(kind)


def setup_inputs(seed: int = 0) -> dict:
    arg_keys = jax.random.split(jax.random.key(seed), 12)
    pool_input = normal_values(arg_keys[0], (TOKENS_A, D), 1.0, 6.0, ((0, 8), (1, 4)))
    group_mix = normal_values(arg_keys[1], (GROUPS, GW, GW), GW ** -0.5, 0.25, ((0, 4),))
    group_scale = jnp.clip(1.0 + 0.18 * jax.random.normal(arg_keys[2], (D,), jnp.float32), 0.1, 1.9)
    out_proj = normal_values(arg_keys[3], (D, D), D ** -0.5, 0.125)
    moe_input = normal_values(arg_keys[4], (TOKENS_B, D), 1.0, 6.0, ((0, 32),))
    norm_gain = jnp.clip(1.0 + 0.18 * jax.random.normal(arg_keys[5], (D,), jnp.float32), 0.1, 1.9)
    expert_ids_keys = jax.random.split(jax.random.fold_in(arg_keys[6], 1), TOKENS_B // TOK_B_DEV)
    expert_ids_turns = jax.random.permutation(jax.random.fold_in(arg_keys[6], 3), TOKENS_B // TOK_B_DEV)
    expert_ids = jax.vmap(lambda own, number: shared_out(jax.random.fold_in(arg_keys[6], 2), own, number, TOK_B_DEV, EXPERTS, TOPK, CAP, 2))(expert_ids_keys, expert_ids_turns).reshape((TOKENS_B, TOPK))
    expert_scores = jnp.clip(jnp.exp(math.log(1.0) - 2.3025851 * jax.random.uniform(arg_keys[7], (TOKENS_B, TOPK), jnp.float32) ** block_levels(arg_keys[7], (TOKENS_B, TOPK), ((0, 32),), -0.2, 0.2)), 0.1, 1.0)
    gate_proj = normal_values(arg_keys[8], (EXPERTS, D, FF), D ** -0.5, 0.125, ((0, 32),))
    up_proj = normal_values(arg_keys[9], (EXPERTS, D, FF), D ** -0.5, 0.125, ((0, 32),))
    down_proj = normal_values(arg_keys[10], (EXPERTS, FF, D), FF ** -0.5, 0.1875, ((0, 32),))
    return dict(pool_input=pool_input, group_mix=group_mix, group_scale=group_scale, out_proj=out_proj, moe_input=moe_input, norm_gain=norm_gain, expert_ids=expert_ids, expert_scores=expert_scores, gate_proj=gate_proj, up_proj=up_proj, down_proj=down_proj)


epsilon = 1e-06

def pool_reference(pool_input, group_mix, group_scale, out_proj):
    total_rows, model_width = pool_input.shape
    group_count, group_width = (group_mix.shape[0], group_mix.shape[1])
    values = pool_input.astype(jnp.float32)
    running = jnp.concatenate([jnp.zeros((1, model_width), jnp.float32), jnp.cumsum(values, axis=0)], axis=0)
    position = jnp.arange(total_rows)
    pieces = []
    for group_id in range(group_count):
        window_len = 2 ** (group_id + 1)
        col_lower = group_id * group_width
        col_upper = col_lower + group_width
        start_row = jnp.maximum(position + 1 - window_len, 0)
        counted = jnp.minimum(position + 1, window_len).astype(jnp.float32)
        window_sum = running[1:, col_lower:col_upper] - running[start_row, col_lower:col_upper]
        pooled = (window_sum / counted[:, None] - values[:, col_lower:col_upper]).astype(jnp.bfloat16)
        grouped = jnp.dot(pooled, group_mix[group_id], preferred_element_type=jnp.float32)
        pieces.append((grouped * group_scale[col_lower:col_upper]).astype(jnp.bfloat16))
    hidden = jnp.concatenate(pieces, axis=1)
    return jnp.dot(hidden, out_proj, preferred_element_type=jnp.float32).astype(jnp.bfloat16)

def expert_reference(moe_input, norm_gain, expert_ids, expert_scores, gate_proj, up_proj, down_proj):
    total_rows, model_width = moe_input.shape
    top_count = expert_ids.shape[1]
    experts_all = gate_proj.shape[0]
    span_rows = N_EP * N_TP * CAP
    values = moe_input.astype(jnp.float32)
    normed = (values * lax.rsqrt(lax.optimization_barrier(jnp.mean(values * values, axis=1, keepdims=True)) + epsilon) * norm_gain).astype(jnp.bfloat16)
    flat_ids = expert_ids.reshape(-1).astype(jnp.int32)
    order_idx = jnp.argsort(flat_ids, stable=True).astype(jnp.int32)
    sorted_ids = flat_ids[order_idx]
    counts = lax.optimization_barrier(jnp.sum((flat_ids[:, None] == jnp.arange(experts_all).astype(jnp.int32)[None, :]).astype(jnp.int32), axis=0)).astype(jnp.int32)
    starts = (jnp.cumsum(counts) - counts).astype(jnp.int32)
    sorted_rows = jnp.concatenate([normed[order_idx // top_count], jnp.zeros((span_rows, model_width), jnp.bfloat16)], axis=0)

    def one_expert(expert_idx):
        rows_in = lax.dynamic_slice_in_dim(sorted_rows, starts[expert_idx], span_rows, 0)
        gate_part = jnp.dot(rows_in, gate_proj[expert_idx], preferred_element_type=jnp.float32)
        up_part = jnp.dot(rows_in, up_proj[expert_idx], preferred_element_type=jnp.float32)
        active = (jax.nn.silu(gate_part) * up_part).astype(jnp.bfloat16)
        return jnp.dot(active, down_proj[expert_idx], preferred_element_type=jnp.float32).astype(jnp.bfloat16)
    outputs = lax.map(one_expert, jnp.arange(experts_all).astype(jnp.int32))
    slot_rank = (jnp.arange(flat_ids.shape[0]).astype(jnp.int32) - starts[sorted_ids]).astype(jnp.int32)
    sorted_out = outputs[sorted_ids, slot_rank]
    per_assign = jnp.zeros((flat_ids.shape[0], model_width), jnp.bfloat16).at[order_idx].set(sorted_out)
    picked = per_assign.astype(jnp.float32).reshape(total_rows, top_count, model_width)
    scores = expert_scores.astype(jnp.float32)
    weights = scores / lax.optimization_barrier(jnp.sum(scores, axis=1, keepdims=True))
    return lax.optimization_barrier(jnp.sum(picked * weights[:, :, None], axis=1)).astype(jnp.bfloat16)

def reference(pool_input, group_mix, group_scale, out_proj, moe_input, norm_gain, expert_ids, expert_scores, gate_proj, up_proj, down_proj):
    mixed_tokens = pool_reference(pool_input, group_mix, group_scale, out_proj)
    mixed_experts = expert_reference(moe_input, norm_gain, expert_ids, expert_scores, gate_proj, up_proj, down_proj)
    return (mixed_tokens, mixed_experts)
```

```python
import jax
import jax.numpy as jnp
from jax import lax
from jax.sharding import PartitionSpec as P

epsilon = 1e-06


def shifted(value, axis, steps):
    count = lax.axis_size(axis)
    first, last = (max(0, -steps), min(count, count - steps))
    return lax.ppermute(value, axis, [(source, source + steps) for source in range(first, last)])


def window_sums(extended, length, halo_depth):
    options = []
    running = extended
    stride = 1
    for level_idx in range(4):
        running = running[stride:] + running[:-stride]
        stride = stride * 2
        offset = halo_depth - (stride - 1)
        options.append(running[offset : offset + length])
    return options


def pool_groups(pool_input, group_mix, group_scale):
    halo_depth = 15
    tok_rows = pool_input.shape[0]
    local_groups, group_width = (group_mix.shape[0], group_mix.shape[1])
    previous = shifted(pool_input[tok_rows - halo_depth :], "ep", 1)
    extended = jnp.concatenate([previous, pool_input], axis=0).astype(jnp.float32)
    options = window_sums(extended, tok_rows, halo_depth)
    position = lax.axis_index("ep") * tok_rows + lax.iota(jnp.int32, tok_rows)
    first_group = lax.axis_index("tp") * local_groups
    group_id = first_group + 0
    trailing = jnp.zeros((tok_rows, group_width), jnp.float32)
    for level_idx in range(4):
        trailing = trailing + jnp.where(group_id == level_idx, options[level_idx], 0.0)
    window_len = jnp.left_shift(jnp.int32(2), group_id)
    counted = jnp.minimum(position + 1, window_len).astype(jnp.float32)
    pooled = (trailing / counted[:, None] - extended[halo_depth:, 0:group_width]).astype(
        jnp.bfloat16
    )
    grouped = jnp.dot(pooled, group_mix[0], preferred_element_type=jnp.float32)
    pieces = (grouped * group_scale).astype(jnp.bfloat16)
    return pieces


def expert_block(received, gate_proj, up_proj, down_proj):
    local_experts = gate_proj.shape[0]
    sources, rows, width = received.shape
    slot_grid = received.reshape(sources // local_experts, local_experts, rows, width)
    results = []
    for j in range(local_experts):
        slots = slot_grid[:, j].reshape(-1, width)
        gate_part = jnp.dot(slots, gate_proj[j], preferred_element_type=jnp.float32)
        up_part = jnp.dot(slots, up_proj[j], preferred_element_type=jnp.float32)
        active = (jax.nn.silu(gate_part) * up_part).astype(jnp.bfloat16)
        result = jnp.dot(active, down_proj[j], preferred_element_type=jnp.float32)
        results.append(result.astype(jnp.bfloat16).reshape(-1, 1, rows, width))
    return jnp.concatenate(results, axis=1).reshape(received.shape)


def slot_targets(expert_ids, experts_all, capacity):
    tok_rows, top_count = expert_ids.shape
    experts = lax.iota(jnp.int32, experts_all)[None, :]
    chosen = [expert_ids[:, k : k + 1] == experts for k in range(top_count)]
    named = sum(pick.astype(jnp.bfloat16) for pick in chosen)
    rows = lax.iota(jnp.int32, tok_rows)
    before = (rows[:, None] > rows[None, :]).astype(jnp.bfloat16)
    earlier = jnp.dot(before, named, preferred_element_type=jnp.float32)
    targets = []
    for k in range(top_count):
        slot = jnp.sum(jnp.where(chosen[k], earlier, 0.0), axis=1).astype(jnp.int32)
        targets.append(expert_ids[:, k] * capacity + slot)
    return targets


def route_experts(moe_input, norm_gain, expert_ids, expert_scores, gate_proj, up_proj, down_proj):
    tok_rows, model_width = moe_input.shape
    top_count = expert_ids.shape[1]
    experts_all = lax.axis_size("ep") * lax.axis_size("tp") * gate_proj.shape[0]
    capacity = 2 * tok_rows * top_count // experts_all
    values = moe_input.astype(jnp.float32)
    normed = (
        values * lax.rsqrt(jnp.mean(values * values, axis=1, keepdims=True) + epsilon) * norm_gain
    ).astype(jnp.bfloat16)
    targets = slot_targets(expert_ids, experts_all, capacity)
    slots = lax.iota(jnp.int32, experts_all * capacity)
    fill = sum((slots[:, None] == t[None, :]).astype(jnp.bfloat16) for t in targets)
    outbound = jnp.dot(fill, normed, preferred_element_type=jnp.float32).astype(jnp.bfloat16)
    outbound = outbound.reshape(experts_all, capacity, model_width)
    returned = lax.all_to_all(
        expert_block(
            lax.all_to_all(outbound, ("ep", "tp"), split_axis=0, concat_axis=0, tiled=True),
            gate_proj,
            up_proj,
            down_proj,
        ),
        ("ep", "tp"),
        split_axis=0,
        concat_axis=0,
        tiled=True,
    ).reshape(experts_all * capacity, model_width)
    weights = expert_scores / jnp.sum(expert_scores, axis=1, keepdims=True)
    spread = sum(
        jnp.where(slots[None, :] == targets[k][:, None], weights[:, k : k + 1], 0.0)
        for k in range(top_count)
    )
    coarse = lax.reduce_precision(spread, 8, 7)
    fine = (spread - coarse).astype(jnp.bfloat16)
    mixed = jnp.dot(coarse.astype(jnp.bfloat16), returned, preferred_element_type=jnp.float32)
    mixed = mixed + jnp.dot(fine, returned, preferred_element_type=jnp.float32)
    return mixed.astype(jnp.bfloat16)


def exchange_groups(hidden):
    count = lax.axis_size("tp")
    me = lax.axis_index("tp")
    rows, width = hidden.shape[0] // count, hidden.shape[1]
    gathered = jnp.zeros((rows, count * width), hidden.dtype)
    for step in range(count):
        dest, source = lax.rem(me + step, count), lax.rem(me + count - step, count)
        block = lax.dynamic_slice_in_dim(hidden, dest * rows, rows, 0)
        if step:
            block = lax.ppermute(block, "tp", [(i, (i + step) % count) for i in range(count)])
        gathered = lax.dynamic_update_slice(gathered, block, (0, source * width))
    return gathered


def body(
    pool_input,
    group_mix,
    group_scale,
    out_proj,
    moe_input,
    norm_gain,
    expert_ids,
    expert_scores,
    gate_proj,
    up_proj,
    down_proj,
):
    hidden = pool_groups(pool_input, group_mix, group_scale)
    gathered = exchange_groups(hidden)
    mixed_tokens = jnp.dot(gathered, out_proj, preferred_element_type=jnp.float32).astype(
        jnp.bfloat16
    )
    mixed_experts = route_experts(
        moe_input, norm_gain, expert_ids, expert_scores, gate_proj, up_proj, down_proj
    )
    return (mixed_tokens, mixed_experts)


def solution(mesh):
    placed = (
        P("ep", "tp"),
        P("tp", None, None),
        P("tp"),
        P(),
        P(("ep", "tp"), None),
        P(),
        P(("ep", "tp"), None),
        P(("ep", "tp"), None),
        P(("ep", "tp"), None, None),
        P(("ep", "tp"), None, None),
        P(("ep", "tp"), None, None),
    )
    return jax.shard_map(
        body,
        mesh=mesh,
        in_specs=placed,
        out_specs=(P(("ep", "tp"), None), P(("ep", "tp"), None)),
        check_vma=False,
    )
```

```python
import functools

import jax
import jax.numpy as jnp
from jax import lax
from jax.experimental import pallas as pl
from jax.experimental.pallas import tpu as pltpu
from jax.sharding import PartitionSpec as P

epsilon = 1e-06


def shifted(value, axis, steps):
    count = lax.axis_size(axis)
    first, last = (max(0, -steps), min(count, count - steps))
    return lax.ppermute(value, axis, [(source, source + steps) for source in range(first, last)])


def window_sums(extended, length, halo_depth):
    options = []
    running = extended
    stride = 1
    for level_idx in range(4):
        running = running[stride:] + running[:-stride]
        stride = stride * 2
        offset = halo_depth - (stride - 1)
        options.append(running[offset : offset + length])
    return options


def pool_groups(pool_input, group_mix, group_scale):
    halo_depth = 15
    tok_rows = pool_input.shape[0]
    local_groups, group_width = (group_mix.shape[0], group_mix.shape[1])
    previous = shifted(pool_input[tok_rows - halo_depth :], "ep", 1)
    extended = jnp.concatenate([previous, pool_input], axis=0).astype(jnp.float32)
    options = window_sums(extended, tok_rows, halo_depth)
    position = lax.axis_index("ep") * tok_rows + lax.iota(jnp.int32, tok_rows)
    first_group = lax.axis_index("tp") * local_groups
    group_id = first_group + 0
    trailing = jnp.zeros((tok_rows, group_width), jnp.float32)
    for level_idx in range(4):
        trailing = trailing + jnp.where(group_id == level_idx, options[level_idx], 0.0)
    window_len = jnp.left_shift(jnp.int32(2), group_id)
    counted = jnp.minimum(position + 1, window_len).astype(jnp.float32)
    pooled = (trailing / counted[:, None] - extended[halo_depth:, 0:group_width]).astype(
        jnp.bfloat16
    )
    grouped = jnp.dot(pooled, group_mix[0], preferred_element_type=jnp.float32)
    pieces = (grouped * group_scale).astype(jnp.bfloat16)
    return pieces


def expert_block(received, gate_proj, up_proj, down_proj):
    local_experts = gate_proj.shape[0]
    sources, rows, width = received.shape
    slot_grid = received.reshape(sources // local_experts, local_experts, rows, width)
    results = []
    for j in range(local_experts):
        slots = slot_grid[:, j].reshape(-1, width)
        gate_part = jnp.dot(slots, gate_proj[j], preferred_element_type=jnp.float32)
        up_part = jnp.dot(slots, up_proj[j], preferred_element_type=jnp.float32)
        active = (jax.nn.silu(gate_part) * up_part).astype(jnp.bfloat16)
        result = jnp.dot(active, down_proj[j], preferred_element_type=jnp.float32)
        results.append(result.astype(jnp.bfloat16).reshape(-1, 1, rows, width))
    return jnp.concatenate(results, axis=1).reshape(received.shape)


def send_experts_kernel(
    n_tp, total, cap, chunks,
    slots, gate_hbm, up_hbm, down_hbm, landed,
    gate, up, down, active, outgoing, load_sem, send_sem, recv_sem,
):
    loads = [
        pltpu.make_async_copy(source.at[0], dest, load_sem.at[i])
        for i, (source, dest) in enumerate(((gate_hbm, gate), (up_hbm, up), (down_hbm, down)))
    ]
    for load in loads:
        load.start()
    me = lax.axis_index("ep") * n_tp + lax.axis_index("tp")
    peers = total // chunks
    rows = peers * cap
    plane, place = lax.div(me, peers), lax.rem(me, peers)
    half = lax.rem(plane + chunks // 2, chunks)
    if chunks == 4:
        order = [half, 3 - plane, 3 - half, plane]
    else:
        order = [lax.rem(plane + c, chunks) for c in range(1, chunks + 1)]
    ff, width = gate.shape[1], gate.shape[0]
    tile_f, tile_n = min(ff, 256), min(width, 512)

    def block(ref, owner):
        return ref.at[pl.ds(pl.multiple_of(owner * cap, cap), cap), :]

    def send(owner):
        return pltpu.make_async_remote_copy(
            src_ref=block(outgoing, owner),
            dst_ref=block(landed, me),
            send_sem=send_sem.at[owner],
            recv_sem=recv_sem.at[me],
            device_id=(lax.div(owner, n_tp), lax.rem(owner, n_tp)),
            device_id_type=pl.DeviceIdType.MESH,
        )

    for c in range(chunks):
        start = pl.multiple_of(order[c] * rows, rows)
        if c == 0:
            loads[0].wait()
            loads[1].wait()

        @pl.loop(0, ff // tile_f)
        def _(i):
            cols = pl.ds(pl.multiple_of(i * tile_f, tile_f), tile_f)
            held = slots[pl.ds(start, rows), :]
            g = jnp.dot(held, gate[:, cols], preferred_element_type=jnp.float32)
            u = jnp.dot(held, up[:, cols], preferred_element_type=jnp.float32)
            active[:, cols] = (g / (1.0 + jnp.exp(-g)) * u).astype(jnp.bfloat16)

        if c == 0:
            loads[2].wait()

        @pl.loop(0, width // tile_n)
        def _(i):
            cols = pl.ds(pl.multiple_of(i * tile_n, tile_n), tile_n)
            r = jnp.dot(active[...], down[:, cols], preferred_element_type=jnp.float32)
            outgoing[pl.ds(start, rows), cols] = r.astype(jnp.bfloat16)

        last = c == chunks - 1

        @pl.loop(0, peers - 1 if last else peers)
        def _(q):
            turn = lax.rem(place + 1 + q, peers)
            send(order[c] * peers + turn).start()

    own = pl.ds(pl.multiple_of(me * cap, cap), cap)
    landed[own, :] = outgoing[own, :]

    @pl.loop(1, total)
    def _(i):
        owner = lax.rem(me + i, total)
        send(owner).wait_send()
        pltpu.make_async_remote_copy(
            src_ref=block(outgoing, owner),
            dst_ref=block(landed, owner),
            send_sem=send_sem.at[owner],
            recv_sem=recv_sem.at[owner],
            device_id=(lax.div(owner, n_tp), lax.rem(owner, n_tp)),
            device_id_type=pl.DeviceIdType.MESH,
        ).wait_recv()


def send_experts(received, gate_proj, up_proj, down_proj):
    n_tp = lax.axis_size("tp")
    total, cap, width = received.shape
    chunks = 4 if total % 4 == 0 else 1
    ff = gate_proj.shape[2]
    vmem, anywhere = pl.BlockSpec(memory_space=pltpu.VMEM), pl.BlockSpec(memory_space=pl.ANY)
    slots = received.reshape(total * cap, width)
    return pl.pallas_call(
        functools.partial(send_experts_kernel, n_tp, total, cap, chunks),
        out_shape=jax.ShapeDtypeStruct(slots.shape, jnp.bfloat16),
        in_specs=[vmem, anywhere, anywhere, anywhere],
        out_specs=vmem,
        scratch_shapes=[
            pltpu.VMEM((width, ff), jnp.bfloat16),
            pltpu.VMEM((width, ff), jnp.bfloat16),
            pltpu.VMEM((ff, width), jnp.bfloat16),
            pltpu.VMEM((total // chunks * cap, ff), jnp.bfloat16),
            pltpu.VMEM(slots.shape, jnp.bfloat16),
            pltpu.SemaphoreType.DMA((3,)),
            pltpu.SemaphoreType.DMA((total,)),
            pltpu.SemaphoreType.DMA((total,)),
        ],
        compiler_params=pltpu.CompilerParams(
            has_side_effects=True, vmem_limit_bytes=60 * 1024 * 1024
        ),
    )(slots, gate_proj, up_proj, down_proj)


def slot_targets(expert_ids, experts_all, capacity):
    tok_rows, top_count = expert_ids.shape
    experts = lax.iota(jnp.int32, experts_all)[None, :]
    chosen = [expert_ids[:, k : k + 1] == experts for k in range(top_count)]
    named = sum(pick.astype(jnp.bfloat16) for pick in chosen)
    rows = lax.iota(jnp.int32, tok_rows)
    before = (rows[:, None] > rows[None, :]).astype(jnp.bfloat16)
    earlier = jnp.dot(before, named, preferred_element_type=jnp.float32)
    targets = []
    for k in range(top_count):
        slot = jnp.sum(jnp.where(chosen[k], earlier, 0.0), axis=1).astype(jnp.int32)
        targets.append(expert_ids[:, k] * capacity + slot)
    return targets


def route_experts(mixed_tokens, moe_input, norm_gain, expert_ids, expert_scores, gate_proj, up_proj, down_proj):
    tok_rows, model_width = moe_input.shape
    top_count = expert_ids.shape[1]
    experts_all = lax.axis_size("ep") * lax.axis_size("tp") * gate_proj.shape[0]
    capacity = 2 * tok_rows * top_count // experts_all
    values = moe_input.astype(jnp.float32)
    normed = (
        values * lax.rsqrt(jnp.mean(values * values, axis=1, keepdims=True) + epsilon) * norm_gain
    ).astype(jnp.bfloat16)
    targets = slot_targets(expert_ids, experts_all, capacity)
    slots = lax.iota(jnp.int32, experts_all * capacity)
    fill = sum((slots[:, None] == t[None, :]).astype(jnp.bfloat16) for t in targets)
    outbound = jnp.dot(fill, normed, preferred_element_type=jnp.float32).astype(jnp.bfloat16)
    outbound = outbound.reshape(experts_all, capacity, model_width)
    received = lax.all_to_all(outbound, ("ep", "tp"), split_axis=0, concat_axis=0, tiled=True)
    received, mixed_tokens = lax.optimization_barrier((received, mixed_tokens))
    if capacity % 16 == 0 and gate_proj.shape[0] == 1:
        returned = send_experts(received, gate_proj, up_proj, down_proj)
    else:
        results = expert_block(received, gate_proj, up_proj, down_proj)
        returned = lax.all_to_all(results, ("ep", "tp"), split_axis=0, concat_axis=0, tiled=True)
    returned = returned.reshape(experts_all * capacity, model_width)
    weights = expert_scores / jnp.sum(expert_scores, axis=1, keepdims=True)
    spread = sum(
        jnp.where(slots[None, :] == targets[k][:, None], weights[:, k : k + 1], 0.0)
        for k in range(top_count)
    )
    coarse = lax.reduce_precision(spread, 8, 7)
    fine = (spread - coarse).astype(jnp.bfloat16)
    mixed = jnp.dot(coarse.astype(jnp.bfloat16), returned, preferred_element_type=jnp.float32)
    mixed = mixed + jnp.dot(fine, returned, preferred_element_type=jnp.float32)
    return mixed_tokens, mixed.astype(jnp.bfloat16)


def exchange_groups(hidden):
    count = lax.axis_size("tp")
    me = lax.axis_index("tp")
    rows, width = hidden.shape[0] // count, hidden.shape[1]
    gathered = jnp.zeros((rows, count * width), hidden.dtype)
    for step in range(count):
        dest, source = lax.rem(me + step, count), lax.rem(me + count - step, count)
        block = lax.dynamic_slice_in_dim(hidden, dest * rows, rows, 0)
        if step:
            block = lax.ppermute(block, "tp", [(i, (i + step) % count) for i in range(count)])
        gathered = lax.dynamic_update_slice(gathered, block, (0, source * width))
    return gathered


def body(
    pool_input,
    group_mix,
    group_scale,
    out_proj,
    moe_input,
    norm_gain,
    expert_ids,
    expert_scores,
    gate_proj,
    up_proj,
    down_proj,
):
    hidden = pool_groups(pool_input, group_mix, group_scale)
    gathered = exchange_groups(hidden)
    mixed_tokens = jnp.dot(gathered, out_proj, preferred_element_type=jnp.float32).astype(
        jnp.bfloat16
    )
    return route_experts(
        mixed_tokens, moe_input, norm_gain, expert_ids, expert_scores, gate_proj, up_proj, down_proj
    )


def solution(mesh):
    placed = (
        P("ep", "tp"),
        P("tp", None, None),
        P("tp"),
        P(),
        P(("ep", "tp"), None),
        P(),
        P(("ep", "tp"), None),
        P(("ep", "tp"), None),
        P(("ep", "tp"), None, None),
        P(("ep", "tp"), None, None),
        P(("ep", "tp"), None, None),
    )
    return jax.shard_map(
        body,
        mesh=mesh,
        in_specs=placed,
        out_specs=(P(("ep", "tp"), None), P(("ep", "tp"), None)),
        check_vma=False,
    )
```

```python
import functools

import jax
import jax.numpy as jnp
from jax import lax
from jax.experimental import pallas as pl
from jax.experimental.pallas import tpu as pltpu
from jax.sharding import PartitionSpec as P

epsilon = 1e-06


def shifted(value, axis, steps):
    count = lax.axis_size(axis)
    first, last = (max(0, -steps), min(count, count - steps))
    return lax.ppermute(value, axis, [(source, source + steps) for source in range(first, last)])


def window_sums(extended, length, halo_depth):
    options = []
    running = extended
    stride = 1
    for level_idx in range(4):
        running = running[stride:] + running[:-stride]
        stride = stride * 2
        offset = halo_depth - (stride - 1)
        options.append(running[offset : offset + length])
    return options


def pool_groups(pool_input, group_mix, group_scale):
    halo_depth = 15
    tok_rows = pool_input.shape[0]
    local_groups, group_width = (group_mix.shape[0], group_mix.shape[1])
    previous = shifted(pool_input[tok_rows - halo_depth :], "ep", 1)
    extended = jnp.concatenate([previous, pool_input], axis=0).astype(jnp.float32)
    options = window_sums(extended, tok_rows, halo_depth)
    position = lax.axis_index("ep") * tok_rows + lax.iota(jnp.int32, tok_rows)
    first_group = lax.axis_index("tp") * local_groups
    group_id = first_group + 0
    trailing = jnp.zeros((tok_rows, group_width), jnp.float32)
    for level_idx in range(4):
        trailing = trailing + jnp.where(group_id == level_idx, options[level_idx], 0.0)
    window_len = jnp.left_shift(jnp.int32(2), group_id)
    counted = jnp.minimum(position + 1, window_len).astype(jnp.float32)
    pooled = (trailing / counted[:, None] - extended[halo_depth:, 0:group_width]).astype(
        jnp.bfloat16
    )
    grouped = jnp.dot(pooled, group_mix[0], preferred_element_type=jnp.float32)
    pieces = (grouped * group_scale).astype(jnp.bfloat16)
    return pieces


def expert_block(received, gate_proj, up_proj, down_proj):
    local_experts = gate_proj.shape[0]
    sources, rows, width = received.shape
    slot_grid = received.reshape(sources // local_experts, local_experts, rows, width)
    results = []
    for j in range(local_experts):
        slots = slot_grid[:, j].reshape(-1, width)
        gate_part = jnp.dot(slots, gate_proj[j], preferred_element_type=jnp.float32)
        up_part = jnp.dot(slots, up_proj[j], preferred_element_type=jnp.float32)
        active = (jax.nn.silu(gate_part) * up_part).astype(jnp.bfloat16)
        result = jnp.dot(active, down_proj[j], preferred_element_type=jnp.float32)
        results.append(result.astype(jnp.bfloat16).reshape(-1, 1, rows, width))
    return jnp.concatenate(results, axis=1).reshape(received.shape)


def send_experts_kernel(
    n_tp, total, cap, chunks,
    slots, gathered, gate_hbm, up_hbm, down_hbm, proj_hbm, landed, mixed,
    gate, up, down, proj, active, outgoing, load_sem, send_sem, recv_sem,
):
    loads = [
        pltpu.make_async_copy(source.at[0], dest, load_sem.at[i])
        for i, (source, dest) in enumerate(((gate_hbm, gate), (up_hbm, up), (down_hbm, down)))
    ]
    loads.append(pltpu.make_async_copy(proj_hbm, proj, load_sem.at[3]))
    for load in loads:
        load.start()
    me = lax.axis_index("ep") * n_tp + lax.axis_index("tp")
    barrier = pltpu.get_barrier_semaphore()

    @pl.loop(1, total)
    def _(i):
        other = lax.rem(me + i, total)
        pl.semaphore_signal(
            barrier,
            inc=1,
            device_id=(lax.div(other, n_tp), lax.rem(other, n_tp)),
            device_id_type=pl.DeviceIdType.MESH,
        )

    peers = total // chunks
    rows = peers * cap
    plane, place = lax.div(me, peers), lax.rem(me, peers)
    half = lax.rem(plane + chunks // 2, chunks)
    if chunks == 4:
        order = [half, 3 - plane, 3 - half, plane]
    else:
        order = [lax.rem(plane + c, chunks) for c in range(1, chunks + 1)]
    ff, width = gate.shape[1], gate.shape[0]
    tile_f, tile_n = min(ff, 256), min(width, 512)

    def block(ref, owner):
        return ref.at[pl.ds(pl.multiple_of(owner * cap, cap), cap), :]

    def send(owner):
        return pltpu.make_async_remote_copy(
            src_ref=block(outgoing, owner),
            dst_ref=block(landed, me),
            send_sem=send_sem.at[owner],
            recv_sem=recv_sem.at[me],
            device_id=(lax.div(owner, n_tp), lax.rem(owner, n_tp)),
            device_id_type=pl.DeviceIdType.MESH,
        )

    for c in range(chunks):
        start = pl.multiple_of(order[c] * rows, rows)
        if c == 0:
            loads[0].wait()
            loads[1].wait()

        @pl.loop(0, ff // tile_f)
        def _(i):
            cols = pl.ds(pl.multiple_of(i * tile_f, tile_f), tile_f)
            held = slots[pl.ds(start, rows), :]
            g = jnp.dot(held, gate[:, cols], preferred_element_type=jnp.float32)
            u = jnp.dot(held, up[:, cols], preferred_element_type=jnp.float32)
            active[:, cols] = (g / (1.0 + jnp.exp(-g)) * u).astype(jnp.bfloat16)

        if c == 0:
            loads[2].wait()

        @pl.loop(0, width // tile_n)
        def _(i):
            cols = pl.ds(pl.multiple_of(i * tile_n, tile_n), tile_n)
            r = jnp.dot(active[...], down[:, cols], preferred_element_type=jnp.float32)
            outgoing[pl.ds(start, rows), cols] = r.astype(jnp.bfloat16)

        if c == 0:
            pl.semaphore_wait(barrier, total - 1)
        last = c == chunks - 1

        @pl.loop(0, peers - 1 if last else peers)
        def _(q):
            turn = lax.rem(place + 1 + q, peers)
            send(order[c] * peers + turn).start()

    own = pl.ds(pl.multiple_of(me * cap, cap), cap)
    landed[own, :] = outgoing[own, :]
    loads[3].wait()

    @pl.loop(0, width // tile_n)
    def _(i):
        cols = pl.ds(pl.multiple_of(i * tile_n, tile_n), tile_n)
        r = jnp.dot(gathered[...], proj[:, cols], preferred_element_type=jnp.float32)
        mixed[:, cols] = r.astype(jnp.bfloat16)

    @pl.loop(1, total)
    def _(i):
        owner = lax.rem(me + i, total)
        send(owner).wait_send()
        pltpu.make_async_remote_copy(
            src_ref=block(outgoing, owner),
            dst_ref=block(landed, owner),
            send_sem=send_sem.at[owner],
            recv_sem=recv_sem.at[owner],
            device_id=(lax.div(owner, n_tp), lax.rem(owner, n_tp)),
            device_id_type=pl.DeviceIdType.MESH,
        ).wait_recv()


def send_experts(received, gathered, out_proj, gate_proj, up_proj, down_proj):
    n_tp = lax.axis_size("tp")
    total, cap, width = received.shape
    chunks = 4 if total % 4 == 0 else 1
    ff = gate_proj.shape[2]
    vmem, anywhere = pl.BlockSpec(memory_space=pltpu.VMEM), pl.BlockSpec(memory_space=pl.ANY)
    slots = received.reshape(total * cap, width)
    return pl.pallas_call(
        functools.partial(send_experts_kernel, n_tp, total, cap, chunks),
        out_shape=(
            jax.ShapeDtypeStruct(slots.shape, jnp.bfloat16),
            jax.ShapeDtypeStruct((gathered.shape[0], out_proj.shape[1]), jnp.bfloat16),
        ),
        in_specs=[vmem, vmem] + [anywhere] * 4,
        out_specs=(vmem, vmem),
        scratch_shapes=[
            pltpu.VMEM((width, ff), jnp.bfloat16),
            pltpu.VMEM((width, ff), jnp.bfloat16),
            pltpu.VMEM((ff, width), jnp.bfloat16),
            pltpu.VMEM(out_proj.shape, jnp.bfloat16),
            pltpu.VMEM((total // chunks * cap, ff), jnp.bfloat16),
            pltpu.VMEM(slots.shape, jnp.bfloat16),
            pltpu.SemaphoreType.DMA((4,)),
            pltpu.SemaphoreType.DMA((total,)),
            pltpu.SemaphoreType.DMA((total,)),
        ],
        compiler_params=pltpu.CompilerParams(
            collective_id=0, has_side_effects=True, vmem_limit_bytes=60 * 1024 * 1024
        ),
    )(slots, gathered, gate_proj, up_proj, down_proj, out_proj)


def slot_targets(expert_ids, experts_all, capacity):
    tok_rows, top_count = expert_ids.shape
    experts = lax.iota(jnp.int32, experts_all)[None, :]
    chosen = [expert_ids[:, k : k + 1] == experts for k in range(top_count)]
    named = sum(pick.astype(jnp.bfloat16) for pick in chosen)
    rows = lax.iota(jnp.int32, tok_rows)
    before = (rows[:, None] > rows[None, :]).astype(jnp.bfloat16)
    earlier = jnp.dot(before, named, preferred_element_type=jnp.float32)
    targets = []
    for k in range(top_count):
        slot = jnp.sum(jnp.where(chosen[k], earlier, 0.0), axis=1).astype(jnp.int32)
        targets.append(expert_ids[:, k] * capacity + slot)
    return targets


def body(
    pool_input,
    group_mix,
    group_scale,
    out_proj,
    moe_input,
    norm_gain,
    expert_ids,
    expert_scores,
    gate_proj,
    up_proj,
    down_proj,
):
    tok_rows, model_width = moe_input.shape
    top_count = expert_ids.shape[1]
    experts_all = lax.axis_size("ep") * lax.axis_size("tp") * gate_proj.shape[0]
    capacity = 2 * tok_rows * top_count // experts_all
    values = moe_input.astype(jnp.float32)
    normed = (
        values * lax.rsqrt(jnp.mean(values * values, axis=1, keepdims=True) + epsilon) * norm_gain
    ).astype(jnp.bfloat16)
    targets = slot_targets(expert_ids, experts_all, capacity)
    slots = lax.iota(jnp.int32, experts_all * capacity)
    fill = sum((slots[:, None] == t[None, :]).astype(jnp.bfloat16) for t in targets)
    outbound = jnp.dot(fill, normed, preferred_element_type=jnp.float32).astype(jnp.bfloat16)
    outbound = outbound.reshape(experts_all, capacity, model_width)
    outbound, pool_input = lax.optimization_barrier((outbound, pool_input))
    received = lax.all_to_all(outbound, ("ep", "tp"), split_axis=0, concat_axis=0, tiled=True)
    gathered = exchange_groups(pool_groups(pool_input, group_mix, group_scale))
    received, gathered = lax.optimization_barrier((received, gathered))
    if capacity % 16 == 0 and gate_proj.shape[0] == 1:
        returned, mixed_tokens = send_experts(
            received, gathered, out_proj, gate_proj, up_proj, down_proj
        )
    else:
        results = expert_block(received, gate_proj, up_proj, down_proj)
        returned = lax.all_to_all(results, ("ep", "tp"), split_axis=0, concat_axis=0, tiled=True)
        mixed_tokens = jnp.dot(gathered, out_proj, preferred_element_type=jnp.float32)
        mixed_tokens = mixed_tokens.astype(jnp.bfloat16)
    returned = returned.reshape(experts_all * capacity, model_width)
    weights = expert_scores / jnp.sum(expert_scores, axis=1, keepdims=True)
    spread = sum(
        jnp.where(slots[None, :] == targets[k][:, None], weights[:, k : k + 1], 0.0)
        for k in range(top_count)
    )
    coarse = lax.reduce_precision(spread, 8, 7)
    fine = (spread - coarse).astype(jnp.bfloat16)
    mixed = jnp.dot(coarse.astype(jnp.bfloat16), returned, preferred_element_type=jnp.float32)
    mixed = mixed + jnp.dot(fine, returned, preferred_element_type=jnp.float32)
    return mixed_tokens, mixed.astype(jnp.bfloat16)


def exchange_groups(hidden):
    count = lax.axis_size("tp")
    me = lax.axis_index("tp")
    rows, width = hidden.shape[0] // count, hidden.shape[1]
    gathered = jnp.zeros((rows, count * width), hidden.dtype)
    for step in range(count):
        dest, source = lax.rem(me + step, count), lax.rem(me + count - step, count)
        block = lax.dynamic_slice_in_dim(hidden, dest * rows, rows, 0)
        if step:
            block = lax.ppermute(block, "tp", [(i, (i + step) % count) for i in range(count)])
        gathered = lax.dynamic_update_slice(gathered, block, (0, source * width))
    return gathered


def solution(mesh):
    placed = (
        P("ep", "tp"),
        P("tp", None, None),
        P("tp"),
        P(),
        P(("ep", "tp"), None),
        P(),
        P(("ep", "tp"), None),
        P(("ep", "tp"), None),
        P(("ep", "tp"), None, None),
        P(("ep", "tp"), None, None),
        P(("ep", "tp"), None, None),
    )
    return jax.shard_map(
        body,
        mesh=mesh,
        in_specs=placed,
        out_specs=(P(("ep", "tp"), None), P(("ep", "tp"), None)),
        check_vma=False,
    )
```
